32 devices in a mesh: sp: 8 (over z, y), tp: 4 (over x, core).
Axes of the slice: x: 2, y: 2, z: 4, core: 2. Of those that a mesh axis runs over, the one named last changes fastest.
Arguments:
- tokens: bfloat16 [1024, 6, 2048], P(('sp', 'tp')), may hold values from -6 to 6
- norm_gain: float32 [2048], replicated, may hold values from 0.1 to 1.9
- w_query: bfloat16 [3, 2048, 1024], P(None, 'sp', 'tp'), may hold values from -0.125 to 0.125
- w_key: bfloat16 [3, 2048, 1024], P(None, 'sp', 'tp'), may hold values from -0.125 to 0.125
- w_value: bfloat16 [3, 2048, 1024], P(None, 'sp', 'tp'), may hold values from -0.125 to 0.125
- w_out: bfloat16 [1024, 2048], P('tp', 'sp'), may hold values from -0.1875 to 0.1875
Outputs:
- mixed: bfloat16 [1024, 6, 2048], P(('sp', 'tp'))
- log_weight: float32 [1024, 6, 8], P('sp', None, 'tp')
The draws below stay inside these ranges and needn't reach their ends.
All inputs are finite; a program needn't handle non-finite values.
Results may differ from the reference program's by a relative error of at most 0.015.
Values may be sent and summed in bfloat16 or wider, within the bound.
A program may use at most 128 MiB of HBM per device.

```python
import jax
import jax.numpy as jnp
from jax import lax

WIDTH = 2048
GROUPS = 3
HEADS = 8
HEAD_WIDTH = 128
STEPS = 24
DILATION_MIDDLE = 4
DILATION_WIDE = 16
BATCH = 6
LENGTH = 1024


def shard_levels(own_key, dims, pieces, least, high):
    def one(dim, blocks):
        draws = jax.random.uniform(jax.random.fold_in(jax.random.fold_in(own_key, 6), dim), (blocks,), jnp.float32, least / len(pieces), high / len(pieces))
        return jnp.repeat(jnp.exp(draws), dims[dim] // blocks).reshape((-1,) + (1,) * (len(dims) - dim - 1))

    factor_of = one(*pieces[0])
    for cut in pieces[1:]:
        factor_of = factor_of * one(*cut)
    return factor_of


def normal_values(rng, dims, spread, limit, cuts=(), kind=jnp.bfloat16):
    array = jax.random.normal(rng, dims, jnp.float32) * spread
    if len(cuts) > 0:
        array = shard_levels(rng, dims, cuts, -0.22, 0.18) * array
    return jnp.clip(array, min=-limit, max=limit).astype(kind)


def setup_inputs(seed: int = 0) -> dict:
    splits = jax.random.split(jax.random.key(seed), 7)
    tokens = normal_values(splits[0], (LENGTH, BATCH, WIDTH), 1.0, 6.0, ((0, 32),))
    norm_gain = jnp.clip(1.0 + 0.18 * jax.random.normal(splits[1], (WIDTH,), jnp.float32), 0.1, 1.9)
    w_query = normal_values(splits[2], (GROUPS, WIDTH, HEADS * HEAD_WIDTH), WIDTH ** -0.5, 0.125, ((1, 8), (2, 4)))
    w_key = normal_values(splits[3], (GROUPS, WIDTH, HEADS * HEAD_WIDTH), WIDTH ** -0.5, 0.125, ((1, 8), (2, 4)))
    w_value = normal_values(splits[4], (GROUPS, WIDTH, HEADS * HEAD_WIDTH), WIDTH ** -0.5, 0.125, ((1, 8), (2, 4)))
    w_out = normal_values(splits[5], (HEADS * HEAD_WIDTH, WIDTH), (HEADS * HEAD_WIDTH) ** -0.5, 0.1875, ((0, 4), (1, 8)))
    return dict(tokens=tokens, norm_gain=norm_gain, w_query=w_query, w_key=w_key, w_value=w_value, w_out=w_out)


epsilon = 1e-06

def rms_normed(values, gain):
    widened = values.astype(jnp.float32)
    scaled = widened * lax.rsqrt(lax.optimization_barrier(jnp.mean(widened * widened, axis=-1, keepdims=True)) + epsilon)
    return (scaled * gain.astype(jnp.float32)).astype(jnp.bfloat16)

def reference(tokens, norm_gain, w_query, w_key, w_value, w_out):
    seq_count, batch_count, width_count = tokens.shape
    normed = rms_normed(tokens, norm_gain)
    flat_rows = normed.reshape(seq_count * batch_count, width_count)
    positions = jnp.arange(seq_count, dtype=jnp.int32)
    scale = 1.0 / HEAD_WIDTH ** 0.5
    group_logs = []
    group_outs = []
    for group_index, dilation in enumerate((1, DILATION_MIDDLE, DILATION_WIDE)):

        def project(weight):
            product = jnp.dot(flat_rows, weight[group_index], preferred_element_type=jnp.float32)
            return product.astype(jnp.bfloat16).reshape(seq_count, batch_count, HEADS, HEAD_WIDTH).astype(jnp.float32)
        queries = project(w_query)
        keys = project(w_key)
        values = project(w_value)
        score_list = []
        for lag_index in range(STEPS + 1):
            offset = lag_index * dilation
            moved = jnp.pad(keys, ((offset, 0), (0, 0), (0, 0), (0, 0)))[:seq_count]
            score = jnp.einsum('sbhe,sbhe->sbh', queries, moved, precision=lax.Precision.HIGHEST) * scale
            score_list.append(jnp.where((positions >= offset)[:, None, None], score, jnp.float32(-1e+30)))
        scores = jnp.stack(score_list)
        peak = lax.optimization_barrier(jnp.max(scores, axis=0))
        lifted = jnp.exp(scores - peak[None])
        totals = lax.optimization_barrier(jnp.sum(lifted, axis=0))
        group_logs.append(peak + jnp.log(totals))
        probs = (lifted / totals[None]).astype(jnp.bfloat16).astype(jnp.float32)
        accumulated = jnp.zeros((seq_count, batch_count, HEADS, HEAD_WIDTH), jnp.float32)
        for lag_index in range(STEPS + 1):
            offset = lag_index * dilation
            moved = jnp.pad(values, ((offset, 0), (0, 0), (0, 0), (0, 0)))[:seq_count]
            accumulated = accumulated + probs[lag_index][..., None] * moved
        group_outs.append(accumulated.astype(jnp.bfloat16))
    stacked_logs = jnp.stack(group_logs)
    top_log = lax.optimization_barrier(jnp.max(stacked_logs, axis=0))
    log_weight = top_log + jnp.log(lax.optimization_barrier(jnp.sum(jnp.exp(stacked_logs - top_log[None]), axis=0)))
    shares = jax.nn.softmax(stacked_logs, axis=0)
    outputs = jnp.stack(group_outs).astype(jnp.float32)
    combined = lax.optimization_barrier(jnp.sum(shares[..., None] * outputs, axis=0)).astype(jnp.bfloat16)
    combined = combined.reshape(seq_count * batch_count, HEADS * HEAD_WIDTH)
    mixed = jnp.dot(combined, w_out, preferred_element_type=jnp.float32).astype(jnp.bfloat16)
    return (mixed.reshape(seq_count, batch_count, width_count), log_weight)
```

```python
import functools
import math

import jax
import jax.numpy as jnp
from jax import lax
from jax.experimental import pallas as pl
from jax.experimental.pallas import tpu as pltpu
from jax.sharding import PartitionSpec as P

GROUPS = 3
HEADS = 8
STEPS = 24
DILATION_MIDDLE = 4
DILATION_WIDE = 16
DILATIONS = (1, DILATION_MIDDLE, DILATION_WIDE)
MESH = pl.DeviceIdType.MESH
PAIR = 2

epsilon = 1e-06


def rms_normed(values, gain):
    widened = values.astype(jnp.float32)
    scaled = widened * lax.rsqrt(jnp.mean(widened * widened, axis=-1, keepdims=True) + epsilon)
    return (scaled * gain.astype(jnp.float32)).astype(jnp.bfloat16)


def remote(src, dst, send, recv, where):
    return pltpu.make_async_remote_copy(
        src_ref=src, dst_ref=dst, send_sem=send, recv_sem=recv, device_id=where, device_id_type=MESH
    )


def gather_kernel(
    n, m, x_ref, q_ref, k_ref, v_ref, o_ref, xf, qf, kf, vf, of,
    local, up_s, up_r, dn_s, dn_r, y_s, y_r, x_s, x_r, o_s, o_r,
):
    s, t = lax.axis_index("sp"), lax.axis_index("tp")
    nz = n // PAIR
    z, y = lax.div(s, PAIR), lax.rem(s, PAIR)
    partner = {"sp": s + 1 - 2 * y}
    above, below = {"sp": s + PAIR}, {"sp": s - PAIR}
    has_above, has_below = z + 1 < nz, z > 0
    peers = [lax.rem(t + i, m) for i in range(1, m)]
    depth, wide, tall = q_ref.shape[1], o_ref.shape[1], o_ref.shape[0]
    rows = x_ref.shape[1]

    barrier = pltpu.get_barrier_semaphore()
    pl.semaphore_signal(barrier, inc=1, device_id=partner, device_id_type=MESH)
    for peer in peers:
        pl.semaphore_signal(barrier, inc=1, device_id={"tp": peer}, device_id_type=MESH)

    @pl.when(has_above)
    def _():
        pl.semaphore_signal(barrier, inc=1, device_id=above, device_id_type=MESH)

    @pl.when(has_below)
    def _():
        pl.semaphore_signal(barrier, inc=1, device_id=below, device_id_type=MESH)

    pl.semaphore_wait(barrier, m + has_above.astype(jnp.int32) + has_below.astype(jnp.int32))

    fulls = (qf, kf, vf)
    owns = (q_ref, k_ref, v_ref)
    tall_rows = pl.ds(pl.multiple_of(t * tall, tall), tall)

    def weight_block(p, zk, side=None):
        index = zk * PAIR + (y if side is None else side)
        return fulls[p].at[:, pl.ds(pl.multiple_of(index * depth, depth), depth), :]

    def out_pair(zk, owner=None):
        at = tall_rows if owner is None else pl.ds(pl.multiple_of(owner * tall, tall), tall)
        if len(of.shape) == 3:
            return of.at[pl.ds(zk * PAIR, PAIR), at, :]
        return of.at[at, pl.ds(pl.multiple_of(zk * PAIR * wide, PAIR * wide), PAIR * wide)]

    def out_own(index):
        if len(of.shape) == 3:
            return of.at[index, tall_rows, :]
        return of.at[tall_rows, pl.ds(pl.multiple_of(index * wide, wide), wide)]

    def x_rows(owner):
        return xf.at[:, pl.ds(pl.multiple_of(owner * rows, rows), rows), :]

    o_local = pltpu.make_async_copy(o_ref, out_own(s), local.at[3])
    o_local.start()
    o_swap = remote(o_ref, out_own(s), y_s.at[0, 0, 3], y_r.at[0, 0, 3], partner)
    o_swap.start()
    token_sends = []
    for i, peer in enumerate(peers):
        c = remote(x_ref, x_rows(t), x_s.at[i], x_r.at[i], {"tp": peer})
        c.start()
        token_sends.append(c)
    locals_ = [pltpu.make_async_copy(x_ref, x_rows(t), local.at[4])]
    for p in range(3):
        locals_.append(pltpu.make_async_copy(owns[p], weight_block(p, z), local.at[p]))
    for c in locals_:
        c.start()
    o_local.wait()
    o_swap.wait()

    def line(up, k, p):
        zk = z - k if up else z + k
        where = above if up else below
        sems = (up_s, up_r) if up else (dn_s, dn_r)
        if p == 3:
            src = out_pair(zk)
            dst = src
        else:
            dst = weight_block(p, zk)
            src = owns[p] if k == 0 else dst
        return remote(src, dst, sems[0].at[k, p], sems[1].at[k, p], where)

    def sideways(up, k, p):
        zk = z - k if up else z + k
        dst = weight_block(p, zk)
        src = owns[p] if k == 0 else dst
        a = 0 if up else 1
        return remote(src, dst, y_s.at[a, k, p], y_r.at[a, k, p], partner)

    def spread(up, k, i):
        zk = z - k if up else z + k
        a = 0 if up else 1
        return remote(out_pair(zk), out_pair(zk), o_s.at[a, k, i], o_r.at[a, k, i], {"tp": peers[i]})

    def arrival(up, k, p):
        zk = z - k if up else z + k
        sems = (up_s, up_r) if up else (dn_s, dn_r)
        dst = out_pair(zk) if p == 3 else weight_block(p, zk)
        return remote(dst, dst, sems[0].at[k - 1, p], sems[1].at[k - 1, p], below if up else above)

    def present(up, k):
        return z - k >= 0 if up else z + k < nz

    def onward(up, k):
        return jnp.logical_and(present(up, k), has_above if up else has_below)

    for k in range(nz):
        for p in (3, 0, 1, 2):
            for up in (True, False):
                def have(up=up, k=k, p=p):
                    if k > 0:
                        arrival(up, k, p).wait_recv()
                    if k < nz - 1:
                        @pl.when(has_above if up else has_below)
                        def _():
                            line(up, k, p).start()
                    if k > 0 or up:
                        if p == 3:
                            for i in range(m - 1):
                                spread(up, k, i).start()
                        else:
                            sideways(up, k, p).start()
                if k == 0:
                    have()
                else:
                    pl.when(present(up, k))(have)

    for c in locals_:
        c.wait()
    for i in range(m - 1):
        token_sends[i].wait_send()
        sender = lax.rem(t + m - 1 - i, m)
        remote(x_ref, x_rows(sender), x_s.at[i], x_r.at[i], {"tp": sender}).wait_recv()
    for k in range(nz):
        for up in (True, False):
            if k < nz - 1:
                @pl.when(onward(up, k))
                def _(up=up, k=k):
                    for p in range(4):
                        line(up, k, p).wait_send()
            if k > 0 or up:
                @pl.when(present(up, k))
                def _(up=up, k=k):
                    zk = z - k if up else z + k
                    a = 0 if up else 1
                    for p in range(3):
                        sideways(up, k, p).wait_send()
                        came = weight_block(p, zk, 1 - y)
                        remote(came, came, y_s.at[a, k, p], y_r.at[a, k, p], partner).wait_recv()
                    for i in range(m - 1):
                        spread(up, k, i).wait_send()
                        sender = lax.rem(t + m - 1 - i, m)
                        came = out_pair(zk, sender)
                        remote(came, came, o_s.at[a, k, i], o_r.at[a, k, i], {"tp": sender}).wait_recv()


def gather_all(x, wq, wk, wv, wo, n, m):
    nz = n // PAIR
    groups, depth, cols = wq.shape
    full_w = jax.ShapeDtypeStruct((groups, depth * n, cols), wq.dtype)
    tall, wide = wo.shape
    blocked = wide % 128 != 0
    out_shape = (n, tall * m, wide) if blocked else (tall * m, wide * n)
    dma = pltpu.SemaphoreType.DMA
    *gathered, out_full = pl.pallas_call(
        functools.partial(gather_kernel, n, m),
        out_shape=(
            jax.ShapeDtypeStruct((x.shape[0], x.shape[1] * m, x.shape[2]), x.dtype),
            full_w, full_w, full_w,
            jax.ShapeDtypeStruct(out_shape, wo.dtype),
        ),
        in_specs=[pl.BlockSpec(memory_space=pltpu.VMEM)] * 5,
        out_specs=(pl.BlockSpec(memory_space=pl.ANY),) * 5,
        scratch_shapes=[
            dma((5,)), dma((nz, 4)), dma((nz, 4)), dma((nz, 4)), dma((nz, 4)),
            dma((2, nz, 4)), dma((2, nz, 4)), dma((m - 1,)), dma((m - 1,)),
            dma((2, nz, m - 1)), dma((2, nz, m - 1)),
        ],
        compiler_params=pltpu.CompilerParams(collective_id=0, has_side_effects=True),
    )(x, wq, wk, wv, wo)
    if blocked:
        out_full = jnp.transpose(out_full, (1, 0, 2)).reshape(tall * m, wide * n)
    return (*gathered, out_full)


def halo_parts(local_rows):
    parts = []
    for g, dilation in enumerate(DILATIONS):
        reach = STEPS * dilation
        for hop in range(1, -(-reach // local_rows) + 1):
            count = min(local_rows, reach - (hop - 1) * local_rows)
            parts.append((g, hop, count, reach - (hop - 1) * local_rows - count))
    return parts


def halo_kernel(n, k_ref, v_ref, *refs):
    halos, (send, recv) = refs[: 2 * GROUPS], refs[2 * GROUPS :]
    s = lax.axis_index("sp")
    local_rows = k_ref.shape[2]
    parts = halo_parts(local_rows)
    farthest = max(hop for _, hop, _, _ in parts)
    barrier = pltpu.get_barrier_semaphore()
    count = jnp.int32(0)
    for hop in range(1, farthest + 1):
        ahead, behind = s + hop < n, s - hop >= 0

        @pl.when(ahead)
        def _():
            pl.semaphore_signal(barrier, inc=1, device_id={"sp": s + hop}, device_id_type=MESH)

        @pl.when(behind)
        def _():
            pl.semaphore_signal(barrier, inc=1, device_id={"sp": s - hop}, device_id_type=MESH)

        count = count + ahead.astype(jnp.int32) + behind.astype(jnp.int32)
    pl.semaphore_wait(barrier, count)

    def copy(index, role):
        g, hop, rows, at = parts[index]
        src = (k_ref, v_ref)[role].at[g, :, pl.ds(local_rows - rows, rows), :]
        dst = halos[role * GROUPS + g].at[:, pl.ds(at, rows), :]
        return remote(src, dst, send.at[index, role], recv.at[index, role], {"sp": s + hop})

    order = sorted(range(len(parts)), key=lambda i: -parts[i][1])
    for index in order:
        @pl.when(s + parts[index][1] < n)
        def _():
            for role in range(2):
                copy(index, role).start()
    for index in order:
        @pl.when(s + parts[index][1] < n)
        def _():
            for role in range(2):
                copy(index, role).wait_send()

        @pl.when(s - parts[index][1] >= 0)
        def _():
            for role in range(2):
                copy(index, role).wait_recv()


def exchange_halos(keys, values, n):
    _, batch, rows, cols = keys.shape
    shapes = tuple(
        jax.ShapeDtypeStruct((batch, STEPS * d, cols), keys.dtype) for d in DILATIONS
    )
    parts = len(halo_parts(rows))
    return pl.pallas_call(
        functools.partial(halo_kernel, n),
        out_shape=shapes + shapes,
        in_specs=[pl.BlockSpec(memory_space=pl.ANY)] * 2,
        out_specs=(pl.BlockSpec(memory_space=pl.ANY),) * (2 * GROUPS),
        scratch_shapes=[pltpu.SemaphoreType.DMA((parts, 2)), pltpu.SemaphoreType.DMA((parts, 2))],
        compiler_params=pltpu.CompilerParams(collective_id=1, has_side_effects=True),
    )(keys, values)


def attend_kernel(place, q_ref, k_ref, v_ref, *refs):
    halos, (out_ref, log_ref) = refs[: 2 * GROUPS], refs[2 * GROUPS :]
    rows, cols = q_ref.shape[2], q_ref.shape[3]
    heads = log_ref.shape[1]
    width = cols // heads
    start = place[0] * rows
    for h in range(heads):
        lanes = slice(h * width, (h + 1) * width)
        logs, outs = [], []
        for g, dilation in enumerate(DILATIONS):
            reach = STEPS * dilation
            query = q_ref[g, 0, :, lanes]

            def scored(key, first, count):
                score = lax.dot_general(query, key, (((1,), (1,)), ((), ())), preferred_element_type=jnp.float32)
                score = score * (1.0 / math.sqrt(width))
                lag = lax.broadcasted_iota(jnp.int32, (rows, count), 0) - lax.broadcasted_iota(jnp.int32, (rows, count), 1) - first
                at = lax.broadcasted_iota(jnp.int32, (rows, count), 1) + (first + start)
                allowed = (lag >= 0) & (lag <= reach) & ((lag & (dilation - 1)) == 0) & (at >= 0)
                return jnp.where(allowed, score, jnp.float32(-1e30))

            near = scored(k_ref[g, 0, :, lanes], 0, rows)
            far = scored(halos[g][0, :, lanes], -reach, reach)
            peak = jnp.maximum(jnp.max(near, axis=1, keepdims=True), jnp.max(far, axis=1, keepdims=True))
            near, far = jnp.exp(near - peak), jnp.exp(far - peak)
            total = jnp.sum(near, axis=1, keepdims=True) + jnp.sum(far, axis=1, keepdims=True)
            logs.append(peak + jnp.log(total))
            known = lax.broadcasted_iota(jnp.int32, (reach, width), 0) + (start - reach) >= 0
            old = halos[GROUPS + g][0, :, lanes]
            old = jnp.where(known, old.astype(jnp.float32), 0.0).astype(jnp.bfloat16)
            mixed = jnp.dot((near / total).astype(jnp.bfloat16), v_ref[g, 0, :, lanes], preferred_element_type=jnp.float32)
            mixed = mixed + jnp.dot((far / total).astype(jnp.bfloat16), old, preferred_element_type=jnp.float32)
            outs.append(mixed.astype(jnp.bfloat16).astype(jnp.float32))
        top = functools.reduce(jnp.maximum, logs)
        shares = [jnp.exp(log - top) for log in logs]
        whole = sum(shares)
        log_ref[0, h] = top + jnp.log(whole)
        combined = sum((share / whole) * out for share, out in zip(shares, outs))
        out_ref[0, :, lanes] = combined.astype(jnp.bfloat16)


def attend(place, q, k, v, halos, heads):
    groups, batch, rows, cols = q.shape
    main = pl.BlockSpec((groups, 1, rows, cols), lambda b: (0, b, 0, 0))
    halo_specs = [pl.BlockSpec((1, h.shape[1], cols), lambda b: (b, 0, 0)) for h in halos]
    return pl.pallas_call(
        attend_kernel,
        grid=(batch,),
        out_shape=(
            jax.ShapeDtypeStruct((batch, rows, cols), jnp.bfloat16),
            jax.ShapeDtypeStruct((batch, heads, rows, 1), jnp.float32),
        ),
        in_specs=[pl.BlockSpec(memory_space=pltpu.SMEM), main, main, main] + halo_specs,
        out_specs=(
            pl.BlockSpec((1, rows, cols), lambda b: (b, 0, 0)),
            pl.BlockSpec((1, heads, rows, 1), lambda b: (b, 0, 0, 0)),
        ),
    )(place, q, k, v, *halos)


def swap_kernel(m, c_ref, out, local, send, recv):
    t = lax.axis_index("tp")
    rows, cols = out.shape[1], c_ref.shape[2]
    peers = [lax.rem(t + i, m) for i in range(1, m)]
    barrier = pltpu.get_barrier_semaphore()
    for peer in peers:
        pl.semaphore_signal(barrier, inc=1, device_id={"tp": peer}, device_id_type=MESH)
    pl.semaphore_wait(barrier, m - 1)

    def piece(owner):
        return c_ref.at[:, pl.ds(pl.multiple_of(owner * rows, rows), rows), :]

    def place(owner):
        return out.at[:, :, pl.ds(pl.multiple_of(owner * cols, cols), cols)]

    copies = [remote(piece(p), place(t), send.at[i], recv.at[i], {"tp": p}) for i, p in enumerate(peers)]
    for c in copies:
        c.start()
    own = pltpu.make_async_copy(piece(t), place(t), local)
    own.start()
    own.wait()
    for i, c in enumerate(copies):
        c.wait_send()
        sender = lax.rem(t + m - 1 - i, m)
        remote(piece(sender), place(sender), send.at[i], recv.at[i], {"tp": sender}).wait_recv()


def swap_heads(combined, m):
    batch, rows, cols = combined.shape
    dma = pltpu.SemaphoreType.DMA
    return pl.pallas_call(
        functools.partial(swap_kernel, m),
        out_shape=jax.ShapeDtypeStruct((batch, rows // m, cols * m), combined.dtype),
        in_specs=[pl.BlockSpec(memory_space=pltpu.VMEM)],
        out_specs=pl.BlockSpec(memory_space=pltpu.VMEM),
        scratch_shapes=[dma, dma((m - 1,)), dma((m - 1,))],
        compiler_params=pltpu.CompilerParams(collective_id=2, has_side_effects=True),
    )(combined)


def shards(tokens, norm_gain, w_query, w_key, w_value, w_out):
    n, m = lax.axis_size("sp"), lax.axis_size("tp")
    normed = rms_normed(jnp.transpose(tokens, (1, 0, 2)), norm_gain)
    rows, query_full, key_full, value_full, out_full = gather_all(normed, w_query, w_key, w_value, w_out, n, m)

    def project(weight):
        return jnp.einsum("btd,gdc->gbtc", rows, weight, preferred_element_type=jnp.float32).astype(jnp.bfloat16)

    keys, values, queries = project(key_full), project(value_full), project(query_full)
    halos = exchange_halos(keys, values, n)
    place = lax.axis_index("sp").astype(jnp.int32).reshape(1)
    combined, logs = attend(place, queries, keys, values, halos, HEADS // m)
    log_weight = jnp.transpose(logs[..., 0], (2, 0, 1))
    swapped = swap_heads(combined, m)
    mixed = jnp.einsum("btc,cd->btd", swapped, out_full, preferred_element_type=jnp.float32).astype(jnp.bfloat16)
    return (jnp.transpose(mixed, (1, 0, 2)), log_weight)


def solution(mesh):
    in_specs = (
        P(("sp", "tp"), None, None),
        P(),
        P(None, "sp", "tp"),
        P(None, "sp", "tp"),
        P(None, "sp", "tp"),
        P("tp", "sp"),
    )
    out_specs = (P(("sp", "tp"), None, None), P("sp", None, "tp"))
    return jax.shard_map(shards, mesh=mesh, in_specs=in_specs, out_specs=out_specs, check_vma=False)
```

```python
import functools
import math

import jax
import jax.numpy as jnp
from jax import lax
from jax.experimental import pallas as pl
from jax.experimental.pallas import tpu as pltpu
from jax.sharding import PartitionSpec as P

GROUPS = 3
HEADS = 8
STEPS = 24
DILATION_MIDDLE = 4
DILATION_WIDE = 16
DILATIONS = (1, DILATION_MIDDLE, DILATION_WIDE)
MESH = pl.DeviceIdType.MESH
PAIR = 2

epsilon = 1e-06


def rms_normed(values, gain):
    widened = values.astype(jnp.float32)
    scaled = widened * lax.rsqrt(jnp.mean(widened * widened, axis=-1, keepdims=True) + epsilon)
    return (scaled * gain.astype(jnp.float32)).astype(jnp.bfloat16)


def remote(src, dst, send, recv, where):
    return pltpu.make_async_remote_copy(
        src_ref=src, dst_ref=dst, send_sem=send, recv_sem=recv, device_id=where, device_id_type=MESH
    )


def gather_kernel(
    n, m, x_ref, q_ref, k_ref, v_ref, o_ref, xf, qf, kf, vf, of,
    local, up_s, up_r, dn_s, dn_r, y_s, y_r, x_s, x_r, o_s, o_r,
):
    s, t = lax.axis_index("sp"), lax.axis_index("tp")
    nz = n // PAIR
    z, y = lax.div(s, PAIR), lax.rem(s, PAIR)
    partner = {"sp": s + 1 - 2 * y}
    above, below = {"sp": s + PAIR}, {"sp": s - PAIR}
    has_above, has_below = z + 1 < nz, z > 0
    peers = [lax.rem(t + i, m) for i in range(1, m)]
    depth, wide, tall = q_ref.shape[1], o_ref.shape[1], o_ref.shape[0]
    rows = x_ref.shape[1]

    barrier = pltpu.get_barrier_semaphore()
    pl.semaphore_signal(barrier, inc=1, device_id=partner, device_id_type=MESH)
    for peer in peers:
        pl.semaphore_signal(barrier, inc=1, device_id={"tp": peer}, device_id_type=MESH)

    @pl.when(has_above)
    def _():
        pl.semaphore_signal(barrier, inc=1, device_id=above, device_id_type=MESH)

    @pl.when(has_below)
    def _():
        pl.semaphore_signal(barrier, inc=1, device_id=below, device_id_type=MESH)

    pl.semaphore_wait(barrier, m + has_above.astype(jnp.int32) + has_below.astype(jnp.int32))

    fulls = (qf, kf, vf)
    owns = (q_ref, k_ref, v_ref)
    tall_rows = pl.ds(pl.multiple_of(t * tall, tall), tall)

    def weight_block(p, zk, side=None):
        index = zk * PAIR + (y if side is None else side)
        return fulls[p].at[:, pl.ds(pl.multiple_of(index * depth, depth), depth), :]

    def out_pair(zk, owner=None):
        at = tall_rows if owner is None else pl.ds(pl.multiple_of(owner * tall, tall), tall)
        if len(of.shape) == 3:
            return of.at[pl.ds(zk * PAIR, PAIR), at, :]
        return of.at[at, pl.ds(pl.multiple_of(zk * PAIR * wide, PAIR * wide), PAIR * wide)]

    def out_own(index):
        if len(of.shape) == 3:
            return of.at[index, tall_rows, :]
        return of.at[tall_rows, pl.ds(pl.multiple_of(index * wide, wide), wide)]

    def x_rows(owner):
        return xf.at[:, pl.ds(pl.multiple_of(owner * rows, rows), rows), :]

    o_local = pltpu.make_async_copy(o_ref, out_own(s), local.at[3])
    o_local.start()
    o_swap = remote(o_ref, out_own(s), y_s.at[0, 0, 3], y_r.at[0, 0, 3], partner)
    o_swap.start()
    token_sends = []
    for i, peer in enumerate(peers):
        c = remote(x_ref, x_rows(t), x_s.at[i], x_r.at[i], {"tp": peer})
        c.start()
        token_sends.append(c)
    locals_ = [pltpu.make_async_copy(x_ref, x_rows(t), local.at[4])]
    for p in range(3):
        locals_.append(pltpu.make_async_copy(owns[p], weight_block(p, z), local.at[p]))
    for c in locals_:
        c.start()
    o_local.wait()
    o_swap.wait()

    def line(up, k, p):
        zk = z - k if up else z + k
        where = above if up else below
        sems = (up_s, up_r) if up else (dn_s, dn_r)
        if p == 3:
            src = out_pair(zk)
            dst = src
        else:
            dst = weight_block(p, zk)
            src = owns[p] if k == 0 else dst
        return remote(src, dst, sems[0].at[k, p], sems[1].at[k, p], where)

    def sideways(up, k, p):
        zk = z - k if up else z + k
        dst = weight_block(p, zk)
        src = owns[p] if k == 0 else dst
        a = 0 if up else 1
        return remote(src, dst, y_s.at[a, k, p], y_r.at[a, k, p], partner)

    def spread(up, k, i):
        zk = z - k if up else z + k
        a = 0 if up else 1
        return remote(out_pair(zk), out_pair(zk), o_s.at[a, k, i], o_r.at[a, k, i], {"tp": peers[i]})

    def arrival(up, k, p):
        zk = z - k if up else z + k
        sems = (up_s, up_r) if up else (dn_s, dn_r)
        dst = out_pair(zk) if p == 3 else weight_block(p, zk)
        return remote(dst, dst, sems[0].at[k - 1, p], sems[1].at[k - 1, p], below if up else above)

    def present(up, k):
        return z - k >= 0 if up else z + k < nz

    def onward(up, k):
        return jnp.logical_and(present(up, k), has_above if up else has_below)

    for k in range(nz):
        for p in (3, 0, 1, 2):
            for up in (True, False):
                def have(up=up, k=k, p=p):
                    if k > 0:
                        arrival(up, k, p).wait_recv()
                    if k < nz - 1:
                        @pl.when(has_above if up else has_below)
                        def _():
                            line(up, k, p).start()
                    if k > 0 or up:
                        if p == 3:
                            for i in range(m - 1):
                                spread(up, k, i).start()
                        else:
                            sideways(up, k, p).start()
                if k == 0:
                    have()
                else:
                    pl.when(present(up, k))(have)

    for c in locals_:
        c.wait()
    for i in range(m - 1):
        token_sends[i].wait_send()
        sender = lax.rem(t + m - 1 - i, m)
        remote(x_ref, x_rows(sender), x_s.at[i], x_r.at[i], {"tp": sender}).wait_recv()
    for k in range(nz):
        for up in (True, False):
            if k < nz - 1:
                @pl.when(onward(up, k))
                def _(up=up, k=k):
                    for p in range(4):
                        line(up, k, p).wait_send()
            if k > 0 or up:
                @pl.when(present(up, k))
                def _(up=up, k=k):
                    zk = z - k if up else z + k
                    a = 0 if up else 1
                    for p in range(3):
                        sideways(up, k, p).wait_send()
                        came = weight_block(p, zk, 1 - y)
                        remote(came, came, y_s.at[a, k, p], y_r.at[a, k, p], partner).wait_recv()
                    for i in range(m - 1):
                        spread(up, k, i).wait_send()
                        sender = lax.rem(t + m - 1 - i, m)
                        came = out_pair(zk, sender)
                        remote(came, came, o_s.at[a, k, i], o_r.at[a, k, i], {"tp": sender}).wait_recv()


def gather_all(x, wq, wk, wv, wo, n, m):
    nz = n // PAIR
    groups, depth, cols = wq.shape
    full_w = jax.ShapeDtypeStruct((groups, depth * n, cols), wq.dtype)
    tall, wide = wo.shape
    blocked = wide % 128 != 0
    out_shape = (n, tall * m, wide) if blocked else (tall * m, wide * n)
    dma = pltpu.SemaphoreType.DMA
    *gathered, out_full = pl.pallas_call(
        functools.partial(gather_kernel, n, m),
        out_shape=(
            jax.ShapeDtypeStruct((x.shape[0], x.shape[1] * m, x.shape[2]), x.dtype),
            full_w, full_w, full_w,
            jax.ShapeDtypeStruct(out_shape, wo.dtype),
        ),
        in_specs=[pl.BlockSpec(memory_space=pltpu.VMEM)] * 5,
        out_specs=(pl.BlockSpec(memory_space=pl.ANY),) * 5,
        scratch_shapes=[
            dma((5,)), dma((nz, 4)), dma((nz, 4)), dma((nz, 4)), dma((nz, 4)),
            dma((2, nz, 4)), dma((2, nz, 4)), dma((m - 1,)), dma((m - 1,)),
            dma((2, nz, m - 1)), dma((2, nz, m - 1)),
        ],
        compiler_params=pltpu.CompilerParams(collective_id=0, has_side_effects=True),
    )(x, wq, wk, wv, wo)
    if blocked:
        out_full = jnp.transpose(out_full, (1, 0, 2)).reshape(tall * m, wide * n)
    return (*gathered, out_full)


def halo_parts(local_rows):
    parts = []
    for g, dilation in enumerate(DILATIONS):
        reach = STEPS * dilation
        for hop in range(1, -(-reach // local_rows) + 1):
            count = min(local_rows, reach - (hop - 1) * local_rows)
            parts.append((g, hop, count, reach - (hop - 1) * local_rows - count))
    return parts


def halo_kernel(n, k_ref, v_ref, *refs):
    halos, (send, recv) = refs[: 2 * GROUPS], refs[2 * GROUPS :]
    s = lax.axis_index("sp")
    local_rows = k_ref.shape[2]
    parts = halo_parts(local_rows)
    farthest = max(hop for _, hop, _, _ in parts)
    barrier = pltpu.get_barrier_semaphore()
    count = jnp.int32(0)
    for hop in range(1, farthest + 1):
        ahead, behind = s + hop < n, s - hop >= 0

        @pl.when(ahead)
        def _():
            pl.semaphore_signal(barrier, inc=1, device_id={"sp": s + hop}, device_id_type=MESH)

        @pl.when(behind)
        def _():
            pl.semaphore_signal(barrier, inc=1, device_id={"sp": s - hop}, device_id_type=MESH)

        count = count + ahead.astype(jnp.int32) + behind.astype(jnp.int32)
    pl.semaphore_wait(barrier, count)

    def copy(index, role):
        g, hop, rows, at = parts[index]
        src = (k_ref, v_ref)[role].at[g, :, pl.ds(local_rows - rows, rows), :]
        dst = halos[role * GROUPS + g].at[:, pl.ds(at, rows), :]
        return remote(src, dst, send.at[index, role], recv.at[index, role], {"sp": s + hop})

    order = sorted(range(len(parts)), key=lambda i: -parts[i][1])
    for index in order:
        @pl.when(s + parts[index][1] < n)
        def _():
            for role in range(2):
                copy(index, role).start()
    for index in order:
        @pl.when(s + parts[index][1] < n)
        def _():
            for role in range(2):
                copy(index, role).wait_send()

        @pl.when(s - parts[index][1] >= 0)
        def _():
            for role in range(2):
                copy(index, role).wait_recv()


def relay_kernel(n, k_ref, v_ref, *refs):
    halos, staged, (send, recv) = refs[: 2 * GROUPS], refs[2 * GROUPS : 2 * GROUPS + 4], refs[2 * GROUPS + 4 :]
    s = lax.axis_index("sp")
    nz = n // PAIR
    z, y = lax.div(s, PAIR), lax.rem(s, PAIR)
    partner, above, below = {"sp": s + 1 - 2 * y}, {"sp": s + PAIR}, {"sp": s - PAIR}
    up, down, down2 = z + 1 < nz, z > 0, z > 1
    local_rows = k_ref.shape[2]
    owns = (k_ref, v_ref)
    wide = GROUPS - 1
    barrier = pltpu.get_barrier_semaphore()
    pl.semaphore_signal(barrier, inc=1, device_id=partner, device_id_type=MESH)

    @pl.when(up)
    def _():
        pl.semaphore_signal(barrier, inc=1, device_id=above, device_id_type=MESH)

    @pl.when(down)
    def _():
        pl.semaphore_signal(barrier, inc=1, device_id=below, device_id_type=MESH)

    pl.semaphore_wait(barrier, 1 + up.astype(jnp.int32) + down.astype(jnp.int32))

    def slot(hop, r):
        return halos[r * GROUPS + wide].at[:, pl.ds((3 - hop) * local_rows, local_rows), :]

    def own(r):
        return owns[r].at[wide]

    def tail(g, r):
        rows = halos[r * GROUPS + g].shape[1]
        return owns[r].at[g, :, pl.ds(local_rows - rows, rows), :]

    def move(src, dst, at, r, where, sent=None):
        return remote(src, dst, send.at[at if sent is None else sent, r], recv.at[at, r], where)

    def landed(hop, r):
        move(slot(hop, r), slot(hop, r), hop, r, partner).wait_recv()

    both = (0, 1)

    def small(r, g, src=None):
        return move(tail(g, r) if src is None else src, halos[r * GROUPS + g], 4 + g, r, partner)

    def lift(r, g):
        return move(tail(g, r), staged[r * 2 + g], 6 + g, r, above)

    def climb(r):
        return move(own(r), slot(2, r), 2, r, above)

    @pl.when(y == 0)
    def _():
        pl.when(up)(lambda: [climb(r).start() for r in both] and None)
        across = [move(own(r), slot(1, r), 1, r, partner) for r in both]
        across += [small(r, g) for g in range(wide) for r in both]
        for c in across:
            c.start()
        side = move(slot(2, 0), slot(3, 0), 3, 0, partner)
        later = [move(slot(1, r), slot(3, r), 3, r, above, 8) for r in both]

        @pl.when(down)
        def _():
            landed(2, 0)
            side.start()
            for r in both:
                landed(1, r)
                pl.when(up)(later[r].start)
            landed(2, 1)
            for g in range(wide):
                for r in both:
                    small(r, g).wait_recv()
            side.wait_send()

            @pl.when(up)
            def _():
                for c in later:
                    c.wait_send()

        @pl.when(down2)
        def _():
            for r in both:
                landed(3, r)

        for c in across:
            c.wait_send()
        pl.when(up)(lambda: [climb(r).wait_send() for r in both] and None)

    @pl.when(y == 1)
    def _():
        @pl.when(up)
        def _():
            for r in both:
                climb(r).start()
            for g in range(wide):
                for r in both:
                    lift(r, g).start()

        over = [move(slot(2, r), slot(1, r), 1, r, partner) for r in both]
        on = move(slot(1, 1), slot(3, 1), 3, 1, above)
        ahead = [small(r, g, staged[r * 2 + g]) for g in range(wide) for r in both]

        @pl.when(down)
        def _():
            for r in both:
                landed(2, r)
                over[r].start()

        for r in both:
            landed(1, r)
        pl.when(up)(on.start)

        @pl.when(down)
        def _():
            for g in range(wide):
                for r in both:
                    lift(r, g).wait_recv()
                    small(r, g, staged[r * 2 + g]).start()
            for r in both:
                landed(3, r)

        for g in range(wide):
            for r in both:
                small(r, g).wait_recv()

        @pl.when(up)
        def _():
            on.wait_send()
            for r in both:
                climb(r).wait_send()
                for g in range(wide):
                    lift(r, g).wait_send()

        @pl.when(down)
        def _():
            for c in over + ahead:
                c.wait_send()


def relay_halos(keys, values, n):
    _, batch, _, cols = keys.shape
    shapes = tuple(
        jax.ShapeDtypeStruct((batch, STEPS * d, cols), keys.dtype) for d in DILATIONS
    )
    outs = shapes + shapes + shapes[:2] + shapes[:2]
    return pl.pallas_call(
        functools.partial(relay_kernel, n),
        out_shape=outs,
        in_specs=[pl.BlockSpec(memory_space=pl.ANY)] * 2,
        out_specs=(pl.BlockSpec(memory_space=pl.ANY),) * len(outs),
        scratch_shapes=[pltpu.SemaphoreType.DMA((9, 2)), pltpu.SemaphoreType.DMA((9, 2))],
        compiler_params=pltpu.CompilerParams(collective_id=1, has_side_effects=True),
    )(keys, values)[: 2 * GROUPS]


def exchange_halos(keys, values, n):
    reaches = [STEPS * d / keys.shape[2] for d in DILATIONS]
    if n % PAIR == 0 and reaches[0] <= 1 and reaches[1] <= 1 and reaches[2] == 3:
        return relay_halos(keys, values, n)
    _, batch, rows, cols = keys.shape
    shapes = tuple(
        jax.ShapeDtypeStruct((batch, STEPS * d, cols), keys.dtype) for d in DILATIONS
    )
    parts = len(halo_parts(rows))
    return pl.pallas_call(
        functools.partial(halo_kernel, n),
        out_shape=shapes + shapes,
        in_specs=[pl.BlockSpec(memory_space=pl.ANY)] * 2,
        out_specs=(pl.BlockSpec(memory_space=pl.ANY),) * (2 * GROUPS),
        scratch_shapes=[pltpu.SemaphoreType.DMA((parts, 2)), pltpu.SemaphoreType.DMA((parts, 2))],
        compiler_params=pltpu.CompilerParams(collective_id=1, has_side_effects=True),
    )(keys, values)


def attend_kernel(place, q_ref, k_ref, v_ref, *refs):
    halos, (out_ref, log_ref) = refs[: 2 * GROUPS], refs[2 * GROUPS :]
    rows, cols = q_ref.shape[2], q_ref.shape[3]
    heads = log_ref.shape[1]
    width = cols // heads
    start = place[0] * rows

    def bias(first, count, dilation):
        lag = lax.broadcasted_iota(jnp.int32, (rows, count), 0) - lax.broadcasted_iota(jnp.int32, (rows, count), 1) - first
        at = lax.broadcasted_iota(jnp.int32, (rows, count), 1) + (first + start)
        return (lag >= 0) & (lag <= STEPS * dilation) & ((lag & (dilation - 1)) == 0) & (at >= 0)

    near_ok = [bias(0, rows, d) for d in DILATIONS]
    far_ok = [bias(-STEPS * d, STEPS * d, d) for d in DILATIONS]
    for h in range(heads):
        lanes = slice(h * width, (h + 1) * width)
        logs, outs = [], []
        for g, dilation in enumerate(DILATIONS):
            reach = STEPS * dilation
            query = q_ref[g, 0, :, lanes]

            def scored(key, allowed):
                score = lax.dot_general(query, key, (((1,), (1,)), ((), ())), preferred_element_type=jnp.float32)
                return jnp.where(allowed, score * (1.0 / math.sqrt(width)), jnp.float32(-1e30))

            near = scored(k_ref[g, 0, :, lanes], near_ok[g])
            far = scored(halos[g][0, :, lanes], far_ok[g])
            peak = jnp.maximum(jnp.max(near, axis=1, keepdims=True), jnp.max(far, axis=1, keepdims=True))
            near, far = jnp.exp(near - peak), jnp.exp(far - peak)
            total = jnp.sum(near, axis=1, keepdims=True) + jnp.sum(far, axis=1, keepdims=True)
            logs.append(peak + jnp.log(total))
            scale = 1.0 / total
            known = lax.broadcasted_iota(jnp.int32, (reach, width), 0) + (start - reach) >= 0
            old = halos[GROUPS + g][0, :, lanes]
            old = jnp.where(known, old.astype(jnp.float32), 0.0).astype(jnp.bfloat16)
            mixed = jnp.dot((near * scale).astype(jnp.bfloat16), v_ref[g, 0, :, lanes], preferred_element_type=jnp.float32)
            mixed = mixed + jnp.dot((far * scale).astype(jnp.bfloat16), old, preferred_element_type=jnp.float32)
            outs.append(mixed.astype(jnp.bfloat16).astype(jnp.float32))
        top = functools.reduce(jnp.maximum, logs)
        shares = [jnp.exp(log - top) for log in logs]
        whole = sum(shares)
        log_ref[0, h] = top + jnp.log(whole)
        combined = sum((share / whole) * out for share, out in zip(shares, outs))
        out_ref[0, :, lanes] = combined.astype(jnp.bfloat16)


def attend(place, q, k, v, halos, heads):
    groups, batch, rows, cols = q.shape
    main = pl.BlockSpec((groups, 1, rows, cols), lambda b: (0, b, 0, 0))
    halo_specs = [pl.BlockSpec((1, h.shape[1], cols), lambda b: (b, 0, 0)) for h in halos]
    return pl.pallas_call(
        attend_kernel,
        grid=(batch,),
        out_shape=(
            jax.ShapeDtypeStruct((batch, rows, cols), jnp.bfloat16),
            jax.ShapeDtypeStruct((batch, heads, rows, 1), jnp.float32),
        ),
        in_specs=[pl.BlockSpec(memory_space=pltpu.SMEM), main, main, main] + halo_specs,
        out_specs=(
            pl.BlockSpec((1, rows, cols), lambda b: (b, 0, 0)),
            pl.BlockSpec((1, heads, rows, 1), lambda b: (b, 0, 0, 0)),
        ),
    )(place, q, k, v, *halos)


def swap_kernel(m, c_ref, out, local, send, recv):
    t = lax.axis_index("tp")
    rows, cols = out.shape[1], c_ref.shape[2]
    peers = [lax.rem(t + i, m) for i in range(1, m)]
    barrier = pltpu.get_barrier_semaphore()
    for peer in peers:
        pl.semaphore_signal(barrier, inc=1, device_id={"tp": peer}, device_id_type=MESH)
    pl.semaphore_wait(barrier, m - 1)

    def piece(owner):
        return c_ref.at[:, pl.ds(pl.multiple_of(owner * rows, rows), rows), :]

    def place(owner):
        return out.at[:, :, pl.ds(pl.multiple_of(owner * cols, cols), cols)]

    copies = [remote(piece(p), place(t), send.at[i], recv.at[i], {"tp": p}) for i, p in enumerate(peers)]
    for c in copies:
        c.start()
    own = pltpu.make_async_copy(piece(t), place(t), local)
    own.start()
    own.wait()
    for i, c in enumerate(copies):
        c.wait_send()
        sender = lax.rem(t + m - 1 - i, m)
        remote(piece(sender), place(sender), send.at[i], recv.at[i], {"tp": sender}).wait_recv()


def swap_heads(combined, m):
    batch, rows, cols = combined.shape
    dma = pltpu.SemaphoreType.DMA
    return pl.pallas_call(
        functools.partial(swap_kernel, m),
        out_shape=jax.ShapeDtypeStruct((batch, rows // m, cols * m), combined.dtype),
        in_specs=[pl.BlockSpec(memory_space=pltpu.VMEM)],
        out_specs=pl.BlockSpec(memory_space=pltpu.VMEM),
        scratch_shapes=[dma, dma((m - 1,)), dma((m - 1,))],
        compiler_params=pltpu.CompilerParams(collective_id=2, has_side_effects=True),
    )(combined)


def shards(tokens, norm_gain, w_query, w_key, w_value, w_out):
    n, m = lax.axis_size("sp"), lax.axis_size("tp")
    normed = rms_normed(jnp.transpose(tokens, (1, 0, 2)), norm_gain)
    rows, query_full, key_full, value_full, out_full = gather_all(normed, w_query, w_key, w_value, w_out, n, m)

    def project(weight):
        return jnp.einsum("btd,gdc->gbtc", rows, weight, preferred_element_type=jnp.float32).astype(jnp.bfloat16)

    keys, values, queries = project(key_full), project(value_full), project(query_full)
    halos = exchange_halos(keys, values, n)
    place = lax.axis_index("sp").astype(jnp.int32).reshape(1)
    combined, logs = attend(place, queries, keys, values, halos, HEADS // m)
    log_weight = jnp.transpose(logs[..., 0], (2, 0, 1))
    swapped = swap_heads(combined, m)
    mixed = jnp.einsum("btc,cd->btd", swapped, out_full, preferred_element_type=jnp.float32).astype(jnp.bfloat16)
    return (jnp.transpose(mixed, (1, 0, 2)), log_weight)


def solution(mesh):
    in_specs = (
        P(("sp", "tp"), None, None),
        P(),
        P(None, "sp", "tp"),
        P(None, "sp", "tp"),
        P(None, "sp", "tp"),
        P("tp", "sp"),
    )
    out_specs = (P(("sp", "tp"), None, None), P("sp", None, "tp"))
    return jax.shard_map(shards, mesh=mesh, in_specs=in_specs, out_specs=out_specs, check_vma=False)
```
